32 devices in a mesh: sp: 4 (over z), fs: 4 (over y, x), tp: 2 (over core).
Axes of the slice: x: 2, y: 2, z: 4, core: 2. Of those that a mesh axis runs over, the one named last changes fastest.
Arguments:
- tokens: bfloat16 [12288, 2048], P(('fs', 'sp'), 'tp'), parts along dimension 0, may hold values from -6 to 6
- norm_gain: bfloat16 [2048], replicated, may hold values from 0.099609375 to 1.8984375
- w_query: bfloat16 [2048, 1024], P(None, 'tp'), may hold values from -0.125 to 0.125
- w_key: bfloat16 [2048, 1024], P(None, 'tp'), may hold values from -0.125 to 0.125
- w_value: bfloat16 [2048, 1024], P(None, 'tp'), may hold values from -0.125 to 0.125
- log_decay: float32 [8, 3072], P('tp', 'sp'), may hold values from -1 to 0
- w_conv_in: bfloat16 [2048, 1024], P(None, 'tp'), may hold values from -0.125 to 0.125
- w_conv_pre: bfloat16 [2048, 1024], P(None, 'tp'), may hold values from -0.125 to 0.125
- w_conv_post: bfloat16 [2048, 1024], P(None, 'tp'), may hold values from -0.125 to 0.125
- conv_taps: bfloat16 [3, 1024], P(None, 'tp'), may hold values from -3 to 3
- w_out_ret: bfloat16 [1024, 2048], replicated, may hold values from -0.125 to 0.125
- w_out_conv: bfloat16 [1024, 2048], replicated, may hold values from -0.125 to 0.125
Outputs:
- mixed: bfloat16 [12288, 2048], P(('fs', 'sp', 'tp')), parts along dimension 0
The draws below stay inside these ranges and needn't reach their ends.
There are 4 independent parts, one for each index of `fs`. The reference program is written for one: setup_inputs(seed, part) draws one part's arguments, and reference() takes and returns one part's arrays. A program takes and returns all parts, laid end to end along the dimension named above; an argument that names none is the same for every part. Nothing has to cross between parts.
All inputs are finite; a program needn't handle non-finite values.
Results may differ from the reference program's by a relative error of at most 0.012.
Values may be sent and summed in bfloat16 or wider, within the bound.
A program may use at most 128 MiB of HBM per device.

```python
import math
import jax
import jax.numpy as jnp
from jax import lax

D = 2048
RETENTION_HEADS = 8
DH = 128
CW = 1024
TAPS = 3
SPAN = 128
TOK_DEV = 768
SEQUENCE_LENGTH = 3072
RW = 1024


def draw_log_decay(key, part):
    head_order = jax.random.permutation(jax.random.fold_in(key, 1), RETENTION_HEADS)
    fast_heads = head_order < RETENTION_HEADS // 2
    token_position = jnp.arange(SEQUENCE_LENGTH, dtype=jnp.int32)
    segment = token_position // TOK_DEV
    jitter = jax.random.uniform(jax.random.fold_in(key, 2), (SEQUENCE_LENGTH // TOK_DEV,), jnp.float32)
    factor = 2.0 ** (1.5 * (segment % 2).astype(jnp.float32) + 0.5 * jitter[segment])
    slow_scale = jax.random.uniform(jax.random.fold_in(key, 3), (RETENTION_HEADS,), jnp.float32, 0.03, 0.09)
    span_length = jax.random.uniform(jax.random.fold_in(key, 4), (RETENTION_HEADS,), jnp.float32, 50.0, 80.0)
    ln_ten = math.log(10.0)
    fast_rate = ln_ten / span_length[:, None] * factor[None, :] * 0.5
    slow_rate = ln_ten * slow_scale[:, None] * factor[None, :] / SEQUENCE_LENGTH
    decay_speed = jnp.where(fast_heads[:, None], fast_rate, slow_rate)
    spike_position = jax.random.randint(jax.random.fold_in(key, 5), (2,), 0, SEQUENCE_LENGTH)
    spike_penalty = jax.random.uniform(jax.random.fold_in(key, 6), (RETENTION_HEADS, 2), jnp.float32, 0.2, 0.4)
    spike_events = jnp.where(token_position[None, :] == spike_position[0], jnp.log1p(-spike_penalty[:, 0:1]), 0.0)
    spike_events = spike_events + jnp.where(token_position[None, :] == spike_position[1], jnp.log1p(-spike_penalty[:, 1:2]), 0.0)
    return (spike_events - decay_speed).astype(jnp.float32)


def steps_of(stream_key, shape, shards, low, largest):
    loudness = 1.0
    for position, shards_of in shards:
        draws = jax.random.uniform(jax.random.fold_in(jax.random.fold_in(stream_key, 6), position), (shards_of,), jnp.float32, low / len(shards), largest / len(shards))
        loudness = loudness * jnp.repeat(jnp.exp(draws), shape[position] // shards_of).reshape((-1,) + (1,) * (len(shape) - 1 - position))
    return loudness


def normal_values(rng, shape, deviation, bound, cuts=(), kind=jnp.bfloat16):
    gain = steps_of(rng, shape, cuts, -0.22, 0.18) if cuts else 1.0
    result = jax.random.normal(rng, shape, jnp.float32) * deviation * gain
    return jnp.minimum(jnp.maximum(result, -bound), bound).astype(kind)


def setup_inputs(seed: int = 0, part: int = 0) -> dict:
    splits = jax.random.split(jax.random.key(seed), 13)
    own_keys = jax.random.split(jax.random.fold_in(splits[12], part), 13)
    return {
        "tokens": normal_values(own_keys[0], (SEQUENCE_LENGTH, D), 1.0, 6.0, ((0, 4), (1, 2))),
        "norm_gain": jnp.clip(1.0 + 0.18 * jax.random.normal(splits[1], (D,), jnp.float32), 0.099609375, 1.8984375).astype(jnp.bfloat16),
        "w_query": normal_values(splits[2], (D, RW), D ** -0.5, 0.125, ((1, 2),)),
        "w_key": normal_values(splits[3], (D, RW), D ** -0.5, 0.125, ((1, 2),)),
        "w_value": normal_values(splits[4], (D, RW), D ** -0.5, 0.125, ((1, 2),)),
        "log_decay": draw_log_decay(jax.random.fold_in(splits[12], 71), part),
        "w_conv_in": normal_values(splits[6], (D, CW), D ** -0.5, 0.125, ((1, 2),)),
        "w_conv_pre": normal_values(splits[7], (D, CW), D ** -0.5, 0.125, ((1, 2),)),
        "w_conv_post": normal_values(splits[8], (D, CW), D ** -0.5, 0.125, ((1, 2),)),
        "conv_taps": normal_values(splits[9], (TAPS, CW), 0.577, 3.0, ((1, 2),)),
        "w_out_ret": normal_values(splits[10], (RW, D), (RW + CW) ** -0.5, 0.125),
        "w_out_conv": normal_values(splits[11], (CW, D), (RW + CW) ** -0.5, 0.125),
    }


epsilon = 1e-06

def rotate(vectors, positions):
    halfway = vectors.shape[-1] // 2
    inverse = 10000.0 ** (-jnp.arange(halfway, dtype=jnp.float32) / halfway)
    angles = positions.astype(jnp.float32)[:, None] * inverse[None, :]
    cosines = jnp.cos(angles)[:, None, :]
    sinusoid = jnp.sin(angles)[:, None, :]
    leading = vectors[..., :halfway]
    trailing = vectors[..., halfway:]
    return jnp.concatenate([leading * cosines - trailing * sinusoid, leading * sinusoid + trailing * cosines], axis=-1)

def retain(queries, keys, values, log_decay):
    blocks = SEQUENCE_LENGTH // SPAN
    query_blocks = queries.reshape(blocks, SPAN, RETENTION_HEADS, DH)
    key_blocks = keys.reshape(blocks, SPAN, RETENTION_HEADS, DH)
    value_blocks = values.reshape(blocks, SPAN, RETENTION_HEADS, DH)
    decay_blocks = log_decay.reshape(RETENTION_HEADS, blocks, SPAN).transpose(1, 0, 2)
    lower_mask = jnp.tril(jnp.ones((SPAN, SPAN), bool))

    def advance(carried, inputs):
        query_block, key_block, value_block, decay_block = inputs
        cumulative = jnp.cumsum(decay_block, axis=-1)
        differences = cumulative[:, :, None] - cumulative[:, None, :]
        decay_weights = jnp.where(lower_mask[None], jnp.exp(jnp.minimum(differences, 0.0)), 0.0)
        query_float = query_block.astype(jnp.float32)
        key_float = key_block.astype(jnp.float32)
        value_float = value_block.astype(jnp.float32)
        scores = jnp.einsum('shd,thd->hst', query_float, key_float)
        mix_weights = lax.optimization_barrier((scores * decay_weights).astype(jnp.bfloat16)).astype(jnp.float32)
        inside = jnp.einsum('hst,thd->shd', mix_weights, value_float)
        across = jnp.einsum('shd,hde->she', query_float, carried, precision=lax.Precision.HIGHEST)
        retained = inside + jnp.exp(cumulative).T[:, :, None] * across
        last_decay = cumulative[:, -1]
        tail_decay = jnp.exp(last_decay[:, None] - cumulative)
        fresh_state = jnp.einsum('shd,she->hde', key_float, value_float * tail_decay.T[:, :, None], precision=lax.Precision.HIGHEST)
        return (jnp.exp(last_decay)[:, None, None] * carried + fresh_state, retained)
    initial = jnp.zeros((RETENTION_HEADS, DH, DH), jnp.float32)
    unused_state, retained = lax.scan(advance, initial, (query_blocks, key_blocks, value_blocks, decay_blocks))
    retained = retained.reshape(SEQUENCE_LENGTH, RETENTION_HEADS, DH)
    normalized = retained * lax.rsqrt(lax.optimization_barrier(jnp.mean(retained * retained, axis=-1, keepdims=True)) + epsilon)
    return normalized.astype(jnp.bfloat16).reshape(SEQUENCE_LENGTH, RETENTION_HEADS * DH)

def reference(tokens, norm_gain, w_query, w_key, w_value, log_decay, w_conv_in, w_conv_pre, w_conv_post, conv_taps, w_out_ret, w_out_conv):
    floats = tokens.astype(jnp.float32)
    normed = (floats * lax.rsqrt(lax.optimization_barrier(jnp.mean(floats * floats, axis=-1, keepdims=True)) + epsilon) * norm_gain.astype(jnp.float32)).astype(jnp.bfloat16)
    positions = jnp.arange(SEQUENCE_LENGTH, dtype=jnp.int32)

    def project(weight):
        return jnp.dot(normed, weight, preferred_element_type=jnp.float32)
    queries = rotate(project(w_query).reshape(SEQUENCE_LENGTH, RETENTION_HEADS, DH), positions).astype(jnp.bfloat16)
    keys = (rotate(project(w_key).reshape(SEQUENCE_LENGTH, RETENTION_HEADS, DH), positions) * DH ** (-0.5)).astype(jnp.bfloat16)
    values = project(w_value).astype(jnp.bfloat16).reshape(SEQUENCE_LENGTH, RETENTION_HEADS, DH)
    ret_out = retain(queries, keys, values, log_decay)
    conv_in = lax.optimization_barrier(project(w_conv_in).astype(jnp.bfloat16))
    conv_pre = lax.optimization_barrier(project(w_conv_pre).astype(jnp.bfloat16))
    conv_post = lax.optimization_barrier(project(w_conv_post).astype(jnp.bfloat16))
    gated_in = (conv_pre.astype(jnp.float32) * conv_in.astype(jnp.float32)).astype(jnp.bfloat16)
    padded = jnp.pad(gated_in, ((TAPS - 1, 0), (0, 0)))
    convolved = jnp.zeros((SEQUENCE_LENGTH, CW), jnp.float32)
    for tap_index in range(TAPS):
        convolved = convolved + conv_taps[tap_index].astype(jnp.float32) * padded[tap_index:tap_index + SEQUENCE_LENGTH].astype(jnp.float32)
    conv_out = (conv_post.astype(jnp.float32) * convolved).astype(jnp.bfloat16)
    mixed_rows = jnp.dot(ret_out, w_out_ret, preferred_element_type=jnp.float32) + jnp.dot(conv_out, w_out_conv, preferred_element_type=jnp.float32)
    return mixed_rows.astype(jnp.bfloat16)
```

```python
import functools

import jax
import jax.numpy as jnp
import numpy as np
from jax import lax
from jax.experimental import pallas as pl
from jax.experimental.pallas import tpu as pltpu
from jax.sharding import PartitionSpec as P

DH = 128
TAPS = 3
SPAN = 128
EPSILON = 1e-06
BF = jnp.bfloat16
F32 = jnp.float32


def dot(a, b, dims=((1,), (0,)), precision=None):
    return lax.dot_general(
        a, b, (dims, ((), ())), preferred_element_type=F32, precision=precision
    )


def kernel(
    sp_count,
    tok_hbm,
    gain_hbm,
    wq_hbm,
    wk_hbm,
    wv_hbm,
    decay_hbm,
    win_hbm,
    wpre_hbm,
    wpost_hbm,
    taps_hbm,
    wor_hbm,
    woc_hbm,
    inner_hbm,
    outer_hbm,
    out_hbm,
    tok,
    normed,
    weights,
    w_ret,
    w_conv,
    gain,
    decay,
    taps,
    inner,
    outer,
    rope_c,
    rope_s,
    cum_row,
    cum_col,
    exp_col,
    tail_col,
    queries,
    keys,
    values,
    post,
    gated,
    starts,
    running,
    state_out,
    state_in,
    incoming,
    inside,
    conv_all,
    conv_in,
    ret_all,
    ret_in,
    total,
    out_vmem,
    load_sem,
    tok_send,
    tok_recv,
    tok_load,
    state_send,
    state_recv,
    pair_send,
    pair_recv,
    rim_send,
    rim_recv,
    out_sem,
):
    rows, half_width = tok_hbm.shape
    width = 2 * half_width
    heads = decay_hbm.shape[0]
    blocks = rows // SPAN
    half = rows // 2
    half_blocks = blocks // 2
    local = heads * DH
    sp = lax.axis_index("sp")
    tp = lax.axis_index("tp")
    other = 1 - tp

    loads = [
        (gain_hbm, gain),
        (decay_hbm, decay),
        (taps_hbm, taps),
        (inner_hbm, inner),
        (outer_hbm.at[sp], outer),
        (wk_hbm, weights.at[0]),
        (wv_hbm, weights.at[1]),
        (wq_hbm, weights.at[2]),
        (win_hbm, weights.at[3]),
        (wpre_hbm, weights.at[4]),
        (wpost_hbm, weights.at[5]),
        (woc_hbm, w_conv),
        (wor_hbm, w_ret),
    ]
    loads = [
        pltpu.make_async_copy(source, target, load_sem.at[i])
        for i, (source, target) in enumerate(loads)
    ]
    (l_gain, l_decay, l_taps, l_inner, l_outer) = loads[:5]
    l_weights = loads[5:11]
    l_woc, l_wor = loads[11:]

    barrier = pltpu.get_barrier_semaphore()
    pl.semaphore_signal(barrier, inc=1, device_id={"tp": other})
    for step in range(1, sp_count):
        pl.semaphore_signal(barrier, inc=1, device_id={"sp": lax.rem(sp + step, sp_count)})

    chunk_rows = [pl.ds(c * half, half) for c in range(2)]
    own_copies = [
        pltpu.make_async_copy(tok_hbm.at[r], tok.at[tp, r], tok_load.at[c])
        for c, r in enumerate(chunk_rows)
    ]
    for copy in loads[:5]:
        copy.start()
    own_copies[0].start()
    own_copies[1].start()
    l_weights[0].start()
    l_weights[1].start()
    pl.semaphore_wait(barrier, sp_count)
    tok_copies = [
        pltpu.make_async_remote_copy(
            src_ref=tok_hbm.at[r],
            dst_ref=tok.at[tp, r],
            send_sem=tok_send.at[c],
            recv_sem=tok_recv.at[c],
            device_id={"tp": other},
        )
        for c, r in enumerate(chunk_rows)
    ]
    for copy in tok_copies:
        copy.start()
    for copy in l_weights[2:]:
        copy.start()
    l_woc.start()
    l_wor.start()

    l_inner.wait()
    l_outer.wait()
    l_decay.wait()
    l_gain.wait()
    row_id = lax.broadcasted_iota(jnp.int32, (SPAN, SPAN), 0)
    col_id = lax.broadcasted_iota(jnp.int32, (SPAN, SPAN), 1)
    lower = row_id >= col_id
    lower_f = jnp.where(lower, 1.0, 0.0)
    for b in range(blocks):
        at = slice(b * SPAN, (b + 1) * SPAN)
        cos_b = outer[0, b : b + 1, :]
        sin_b = outer[1, b : b + 1, :]
        rope_c[at, :] = inner[0] * cos_b - inner[1] * sin_b
        rope_s[at, :] = inner[1] * cos_b + inner[0] * sin_b
        logs = decay[:, at]
        by_row = dot(logs, lower_f, ((1,), (1,)), lax.Precision.HIGHEST)
        by_col = dot(lower_f, logs, ((1,), (1,)), lax.Precision.HIGHEST)
        cum_row[b] = by_row
        cum_col[at, :] = by_col
        exp_col[at, :] = jnp.exp(by_col)
        tail_col[at, :] = jnp.exp(by_col[SPAN - 1 : SPAN, :] - by_col)
    running[...] = jnp.zeros_like(running)
    incoming[...] = jnp.zeros_like(incoming)

    def norm_chunk(c):
        def step(i, _):
            at = pl.ds(pl.multiple_of(c * half + i * 32, 32), 32)
            x0 = tok[0, at, :].astype(F32)
            x1 = tok[1, at, :].astype(F32)
            squares = jnp.sum(x0 * x0 + x1 * x1, axis=-1, keepdims=True)
            scale = lax.rsqrt(squares * (1.0 / width) + EPSILON)
            normed[at, :half_width] = (x0 * scale * gain[:, :half_width].astype(F32)).astype(BF)
            normed[at, half_width:] = (x1 * scale * gain[:, half_width:].astype(F32)).astype(BF)
            return 0

        lax.fori_loop(0, half // 32, step, 0)

    def project(c, which):
        return dot(normed[c * half : (c + 1) * half, :], weights[which])

    def rotate_into(target, product, c, factor):
        for b in range(half_blocks):
            at = slice(c * half + b * SPAN, c * half + (b + 1) * SPAN)
            cosines = rope_c[at, :]
            sines = rope_s[at, :]
            if factor is not None:
                cosines = cosines * factor
                sines = sines * factor
            for h in range(heads):
                x = product[b * SPAN : (b + 1) * SPAN, h * DH : (h + 1) * DH]
                turned = x * cosines + pltpu.roll(x, DH // 2, 1) * sines
                target[at, h * DH : (h + 1) * DH] = turned.astype(BF)

    for c in range(2):
        own_copies[c].wait()
        tok_copies[c].wait_recv()
        norm_chunk(c)
        if c == 0:
            l_weights[0].wait()
            l_weights[1].wait()
        rotate_into(keys, project(c, 0), c, DH**-0.5)
        values[c * half : (c + 1) * half, :] = project(c, 1).astype(BF)

    def state_step(b, _):
        at = pl.ds(pl.multiple_of(b * SPAN, SPAN), SPAN)
        ends = jnp.exp(cum_row[b][:, SPAN - 1 : SPAN])
        for h in range(heads):
            cols = slice(h * DH, (h + 1) * DH)
            weighted = (values[at, cols].astype(F32) * tail_col[at, h : h + 1]).astype(BF)
            fresh = dot(keys[at, cols], weighted, ((0,), (0,)))
            held = running[cols, :]
            starts[b, cols, :] = held
            running[cols, :] = ends[h : h + 1, :] * held + fresh
        return 0

    lax.fori_loop(0, blocks, state_step, 0)
    state_out[0:local, :] = running[...].astype(BF)
    ends_total = cum_row[0][:, SPAN - 1 : SPAN]
    for b in range(1, blocks):
        ends_total = ends_total + cum_row[b][:, SPAN - 1 : SPAN]
    for h in range(heads):
        state_out[local + 16 * h : local + 16 * (h + 1), :] = jnp.broadcast_to(
            jnp.exp(ends_total[h : h + 1, :]), (16, DH)
        ).astype(BF)

    l_weights[2].wait()
    rotate_into(queries, project(0, 2), 0, None)

    def state_copy(step):
        return pltpu.make_async_remote_copy(
            src_ref=state_out,
            dst_ref=state_in.at[step - 1],
            send_sem=state_send.at[step - 1],
            recv_sem=state_recv.at[step - 1],
            device_id={"sp": lax.rem(sp + step, sp_count)},
        )

    for step in range(1, sp_count):
        @pl.when(sp + step < sp_count)
        def _():
            state_copy(step).start()

    rotate_into(queries, project(1, 2), 1, None)

    l_weights[3].wait()
    l_weights[4].wait()
    for c in range(2):
        first = project(c, 3).astype(BF).astype(F32)
        second = project(c, 4).astype(BF).astype(F32)
        gated[8 + c * half : 8 + (c + 1) * half, :] = (first * second).astype(BF).astype(F32)

    @pl.when(sp == 0)
    def _():
        gated[0:8, :] = jnp.zeros((8, local), F32)

    l_weights[5].wait()
    post[0:half, :] = project(0, 5).astype(BF)
    rim_copy = pltpu.make_async_remote_copy(
        src_ref=gated.at[pl.ds(rows, 8)],
        dst_ref=gated.at[pl.ds(0, 8)],
        send_sem=rim_send,
        recv_sem=rim_recv,
        device_id={"sp": lax.rem(sp + 1, sp_count)},
    )

    @pl.when(sp + 1 < sp_count)
    def _():
        rim_copy.start()

    post[half:, :] = project(1, 5).astype(BF)

    def inside_step(b, _):
        at = pl.ds(pl.multiple_of(b * SPAN, SPAN), SPAN)
        row = cum_row[b]
        for h in range(heads):
            cols = slice(h * DH, (h + 1) * DH)
            scores = dot(queries[at, cols], keys[at, cols], ((1,), (1,)))
            gap = jnp.minimum(cum_col[at, h : h + 1] - row[h : h + 1, :], 0.0)
            mix = (scores * jnp.where(lower, jnp.exp(gap), 0.0)).astype(BF)
            inside[at, cols] = dot(mix, values[at, cols])
        return 0

    lax.fori_loop(0, blocks, inside_step, 0)

    @pl.when(sp > 0)
    def _():
        rim_copy.wait_recv()

    l_taps.wait()
    tap = [taps[i : i + 1, :].astype(F32) for i in range(TAPS)]
    for b in range(blocks):
        base = b * SPAN + 8 - (TAPS - 1)
        convolved = tap[0] * gated[base : base + SPAN, :]
        for i in range(1, TAPS):
            convolved = convolved + tap[i] * gated[base + i : base + i + SPAN, :]
        at = slice(b * SPAN, (b + 1) * SPAN)
        conv_all[at, :] = (post[at, :].astype(F32) * convolved).astype(BF)

    def pair_copy(source, target, i):
        return pltpu.make_async_remote_copy(
            src_ref=source.at[pl.ds(pl.multiple_of(other * half, half), half)],
            dst_ref=target,
            send_sem=pair_send.at[i],
            recv_sem=pair_recv.at[i],
            device_id={"tp": other},
        )

    mine = pl.ds(pl.multiple_of(tp * half, half), half)
    my_inputs = pl.ds(pl.multiple_of(tp * local, local), local)
    other_inputs = pl.ds(pl.multiple_of(other * local, local), local)
    tiles = width // 512

    def tile_at(n):
        return pl.ds(pl.multiple_of(n * 512, 512), 512)

    l_woc.wait()
    conv_copy = pair_copy(conv_all, conv_in, 0)
    conv_copy.start()

    def conv_own(n, _):
        total[:, tile_at(n)] = dot(conv_all[mine, :], w_conv[my_inputs, tile_at(n)])
        return 0

    lax.fori_loop(0, tiles, conv_own, 0)
    conv_copy.wait_recv()

    def conv_other(n, _):
        total[:, tile_at(n)] += dot(conv_in[...], w_conv[other_inputs, tile_at(n)])
        return 0

    lax.fori_loop(0, tiles, conv_other, 0)

    for step in range(sp_count - 1, 0, -1):
        @pl.when(sp >= step)
        def _():
            state_copy(step).wait_recv()
            for h in range(heads):
                cols = slice(h * DH, (h + 1) * DH)
                shrink = state_in[step - 1, local + 16 * h : local + 16 * (h + 1), :].astype(F32)
                incoming[cols, :] = (
                    shrink[0:1, :] * incoming[cols, :] + state_in[step - 1, cols, :].astype(F32)
                )

    def across_half(which):
        def step(i, before):
            b = which * half_blocks + i
            at = pl.ds(pl.multiple_of(b * SPAN, SPAN), SPAN)
            factor = jnp.exp(before)
            for h in range(heads):
                cols = slice(h * DH, (h + 1) * DH)
                state = (starts[b, cols, :] + factor[h : h + 1, :] * incoming[cols, :]).astype(BF)
                across = dot(queries[at, cols], state)
                retained = inside[at, cols] + exp_col[at, h : h + 1] * across
                power = jnp.sum(retained * retained, axis=-1, keepdims=True) * (1.0 / DH)
                ret_all[at, cols] = (retained * lax.rsqrt(power + EPSILON)).astype(BF)
            return before + cum_row[b][:, SPAN - 1 : SPAN]

        first_half = cum_row[0][:, SPAN - 1 : SPAN]
        for b in range(1, half_blocks):
            first_half = first_half + cum_row[b][:, SPAN - 1 : SPAN]
        lax.fori_loop(0, half_blocks, step, first_half * which.astype(F32))

    across_half(other)
    ret_copy = pair_copy(ret_all, ret_in, 1)
    ret_copy.start()
    across_half(tp)
    l_wor.wait()

    def ret_own(n, _):
        total[:, tile_at(n)] += dot(ret_all[mine, :], w_ret[my_inputs, tile_at(n)])
        return 0

    lax.fori_loop(0, tiles, ret_own, 0)
    ret_copy.wait_recv()

    def out_copy(n):
        return pltpu.make_async_copy(
            out_vmem.at[:, tile_at(n)], out_hbm.at[:, tile_at(n)], out_sem.at[n]
        )

    def ret_other(n, _):
        final = total[:, tile_at(n)] + dot(ret_in[...], w_ret[other_inputs, tile_at(n)])
        out_vmem[:, tile_at(n)] = final.astype(BF)
        out_copy(n).start()
        return 0

    lax.fori_loop(0, tiles, ret_other, 0)

    for copy in tok_copies:
        copy.wait_send()
    for step in range(1, sp_count):
        @pl.when(sp + step < sp_count)
        def _():
            state_copy(step).wait_send()

    @pl.when(sp + 1 < sp_count)
    def _():
        rim_copy.wait_send()

    conv_copy.wait_send()
    ret_copy.wait_send()
    for n in range(tiles):
        out_copy(n).wait()


def rotation_tables(sp_count, rows):
    halfway = DH // 2
    inverse = 10000.0 ** (-np.arange(halfway, dtype=np.float64) / halfway)
    sign = np.concatenate([-np.ones(halfway), np.ones(halfway)])
    inverse = np.concatenate([inverse, inverse])

    def table(positions):
        angles = positions[:, None] * inverse[None, :]
        return np.stack([np.cos(angles), np.sin(angles) * sign]).astype(np.float32)

    inner = table(np.arange(SPAN))
    blocks = rows // SPAN
    outer = np.zeros((sp_count, 2, -(-blocks // 8) * 8, DH), np.float32)
    for device in range(sp_count):
        outer[device, :, :blocks] = table(SPAN * (device * blocks + np.arange(blocks)))
    return jnp.asarray(inner), jnp.asarray(outer)


def body(
    sp_count,
    tokens,
    norm_gain,
    w_query,
    w_key,
    w_value,
    log_decay,
    w_conv_in,
    w_conv_pre,
    w_conv_post,
    conv_taps,
    w_out_ret,
    w_out_conv,
):
    rows, half_width = tokens.shape
    width = 2 * half_width
    heads = log_decay.shape[0]
    local = heads * DH
    half = rows // 2
    blocks = rows // SPAN
    inner, outer = rotation_tables(sp_count, rows)
    any_spec = pl.BlockSpec(memory_space=pl.ANY)
    vmem, dma = pltpu.VMEM, pltpu.SemaphoreType.DMA
    scratch = [
        vmem((2, rows, half_width), BF),
        vmem((rows, width), BF),
        vmem((6, width, local), BF),
        vmem(w_out_ret.shape, BF),
        vmem(w_out_conv.shape, BF),
        vmem((1, width), BF),
        vmem(log_decay.shape, F32),
        vmem(conv_taps.shape, BF),
        vmem(inner.shape, F32),
        vmem(outer.shape[1:], F32),
        vmem((rows, DH), F32),
        vmem((rows, DH), F32),
        vmem((blocks, heads, SPAN), F32),
        vmem((rows, heads), F32),
        vmem((rows, heads), F32),
        vmem((rows, heads), F32),
        vmem((rows, local), BF),
        vmem((rows, local), BF),
        vmem((rows, local), BF),
        vmem((rows, local), BF),
        vmem((rows + 8, local), F32),
        vmem((blocks, local, DH), F32),
        vmem((local, DH), F32),
        vmem((local + 16 * heads, DH), BF),
        vmem((sp_count - 1, local + 16 * heads, DH), BF),
        vmem((local, DH), F32),
        vmem((rows, local), F32),
        vmem((rows, local), BF),
        vmem((half, local), BF),
        vmem((rows, local), BF),
        vmem((half, local), BF),
        vmem((half, width), F32),
        vmem((half, width), BF),
        dma((13,)),
        dma((2,)),
        dma((2,)),
        dma((2,)),
        dma((sp_count - 1,)),
        dma((sp_count - 1,)),
        dma((2,)),
        dma((2,)),
        dma,
        dma,
        dma((width // 512,)),
    ]
    return pl.pallas_call(
        functools.partial(kernel, sp_count),
        out_shape=jax.ShapeDtypeStruct((half, width), BF),
        in_specs=[any_spec] * 14,
        out_specs=any_spec,
        scratch_shapes=scratch,
        compiler_params=pltpu.CompilerParams(
            collective_id=0, has_side_effects=True, vmem_limit_bytes=60 * 1024 * 1024
        ),
        name="mixer",
    )(
        tokens,
        norm_gain.reshape(1, width),
        w_query,
        w_key,
        w_value,
        log_decay,
        w_conv_in,
        w_conv_pre,
        w_conv_post,
        conv_taps,
        w_out_ret,
        w_out_conv,
        inner,
        outer,
    )


def solution(mesh):
    in_specs = (
        P(("fs", "sp"), "tp"),
        P(),
        P(None, "tp"),
        P(None, "tp"),
        P(None, "tp"),
        P("tp", "sp"),
        P(None, "tp"),
        P(None, "tp"),
        P(None, "tp"),
        P(None, "tp"),
        P(),
        P(),
    )
    out_specs = P(("fs", "sp", "tp"), None)
    return jax.shard_map(
        functools.partial(body, mesh.shape["sp"]),
        mesh=mesh,
        in_specs=in_specs,
        out_specs=out_specs,
        check_vma=False,
    )
```

```python
import functools

import jax
import jax.numpy as jnp
import numpy as np
from jax import lax
from jax.experimental import pallas as pl
from jax.experimental.pallas import tpu as pltpu
from jax.sharding import PartitionSpec as P

DH = 128
TAPS = 3
SPAN = 128
EPSILON = 1e-06
BF = jnp.bfloat16
F32 = jnp.float32


def dot(a, b, dims=((1,), (0,)), precision=None):
    return lax.dot_general(
        a, b, (dims, ((), ())), preferred_element_type=F32, precision=precision
    )


def kernel(
    sp_count,
    tok_hbm,
    gain_hbm,
    wq_hbm,
    wk_hbm,
    wv_hbm,
    decay_hbm,
    win_hbm,
    wpre_hbm,
    wpost_hbm,
    taps_hbm,
    wor_hbm,
    woc_hbm,
    inner_hbm,
    outer_hbm,
    out_vmem,
    tok,
    normed,
    weights,
    w_ret,
    w_conv,
    gain,
    decay,
    taps,
    inner,
    outer,
    rope_c,
    rope_s,
    cum_row,
    cum_col,
    exp_col,
    tail_col,
    queries,
    keys,
    values,
    post,
    gated,
    starts,
    running,
    state_out,
    state_in,
    incoming,
    inside,
    conv_all,
    conv_in,
    ret_all,
    ret_in,
    total,
    load_sem,
    tok_send,
    tok_recv,
    tok_load,
    state_send,
    state_recv,
    pair_send,
    pair_recv,
    rim_send,
    rim_recv,
):
    rows, half_width = tok_hbm.shape
    width = 2 * half_width
    heads = decay_hbm.shape[0]
    blocks = rows // SPAN
    half = rows // 2
    half_blocks = blocks // 2
    local = heads * DH
    sp = lax.axis_index("sp")
    tp = lax.axis_index("tp")
    other = 1 - tp

    loads = [
        (gain_hbm, gain),
        (decay_hbm, decay),
        (taps_hbm, taps),
        (inner_hbm, inner),
        (outer_hbm.at[sp], outer),
        (wk_hbm, weights.at[0]),
        (wv_hbm, weights.at[1]),
        (wq_hbm, weights.at[2]),
        (win_hbm, weights.at[3]),
        (wpre_hbm, weights.at[4]),
        (wpost_hbm, weights.at[5]),
        (woc_hbm, w_conv),
        (wor_hbm, w_ret),
    ]
    loads = [
        pltpu.make_async_copy(source, target, load_sem.at[i])
        for i, (source, target) in enumerate(loads)
    ]
    (l_gain, l_decay, l_taps, l_inner, l_outer) = loads[:5]
    l_weights = loads[5:11]
    l_woc, l_wor = loads[11:]

    barrier = pltpu.get_barrier_semaphore()
    pl.semaphore_signal(barrier, inc=1, device_id={"tp": other})
    for step in range(1, sp_count):
        pl.semaphore_signal(barrier, inc=1, device_id={"sp": lax.rem(sp + step, sp_count)})

    chunk_rows = [pl.ds(c * half, half) for c in range(2)]
    own_copies = [
        pltpu.make_async_copy(tok_hbm.at[r], tok.at[tp, r], tok_load.at[c])
        for c, r in enumerate(chunk_rows)
    ]
    for copy in loads[:5]:
        copy.start()
    own_copies[0].start()
    own_copies[1].start()
    l_weights[0].start()
    l_weights[1].start()
    pl.semaphore_wait(barrier, sp_count)
    tok_copies = [
        pltpu.make_async_remote_copy(
            src_ref=tok_hbm.at[r],
            dst_ref=tok.at[tp, r],
            send_sem=tok_send.at[c],
            recv_sem=tok_recv.at[c],
            device_id={"tp": other},
        )
        for c, r in enumerate(chunk_rows)
    ]
    for copy in tok_copies:
        copy.start()
    for copy in l_weights[2:]:
        copy.start()
    l_woc.start()
    l_wor.start()

    l_inner.wait()
    l_outer.wait()
    l_decay.wait()
    l_gain.wait()
    row_id = lax.broadcasted_iota(jnp.int32, (SPAN, SPAN), 0)
    col_id = lax.broadcasted_iota(jnp.int32, (SPAN, SPAN), 1)
    lower = row_id >= col_id
    lower_f = jnp.where(lower, 1.0, 0.0)
    for b in range(blocks):
        at = slice(b * SPAN, (b + 1) * SPAN)
        cos_b = outer[0, b : b + 1, :]
        sin_b = outer[1, b : b + 1, :]
        rope_c[at, :] = inner[0] * cos_b - inner[1] * sin_b
        rope_s[at, :] = inner[1] * cos_b + inner[0] * sin_b
        logs = decay[:, at]
        by_row = dot(logs, lower_f, ((1,), (1,)), lax.Precision.HIGHEST)
        by_col = dot(lower_f, logs, ((1,), (1,)), lax.Precision.HIGHEST)
        cum_row[b] = by_row
        cum_col[at, :] = by_col
        exp_col[at, :] = jnp.exp(by_col)
        tail_col[at, :] = jnp.exp(by_col[SPAN - 1 : SPAN, :] - by_col)
    gain_row = gain[...].astype(F32).reshape(1, width)
    running[...] = jnp.zeros_like(running)
    incoming[...] = jnp.zeros_like(incoming)

    def norm_chunk(c):
        def step(i, _):
            at = pl.ds(pl.multiple_of(c * half + i * 32, 32), 32)
            x0 = tok[0, at, :].astype(F32)
            x1 = tok[1, at, :].astype(F32)
            squares = jnp.sum(x0 * x0 + x1 * x1, axis=-1, keepdims=True)
            scale = lax.rsqrt(squares * (1.0 / width) + EPSILON)
            normed[at, :half_width] = (x0 * scale * gain_row[:, :half_width]).astype(BF)
            normed[at, half_width:] = (x1 * scale * gain_row[:, half_width:]).astype(BF)
            return 0

        lax.fori_loop(0, half // 32, step, 0)

    def project(c, which):
        return dot(normed[c * half : (c + 1) * half, :], weights[which])

    def rotate_into(target, product, c, factor):
        for b in range(half_blocks):
            at = slice(c * half + b * SPAN, c * half + (b + 1) * SPAN)
            cosines = rope_c[at, :]
            sines = rope_s[at, :]
            if factor is not None:
                cosines = cosines * factor
                sines = sines * factor
            for h in range(heads):
                x = product[b * SPAN : (b + 1) * SPAN, h * DH : (h + 1) * DH]
                turned = x * cosines + pltpu.roll(x, DH // 2, 1) * sines
                target[at, h * DH : (h + 1) * DH] = turned.astype(BF)

    for c in range(2):
        own_copies[c].wait()
        tok_copies[c].wait_recv()
        norm_chunk(c)
        if c == 0:
            l_weights[0].wait()
            l_weights[1].wait()
        rotate_into(keys, project(c, 0), c, DH**-0.5)
        values[c * half : (c + 1) * half, :] = project(c, 1).astype(BF)

    def state_step(b, _):
        at = pl.ds(pl.multiple_of(b * SPAN, SPAN), SPAN)
        ends = jnp.exp(cum_row[b][:, SPAN - 1 : SPAN])
        for h in range(heads):
            cols = slice(h * DH, (h + 1) * DH)
            weighted = (values[at, cols].astype(F32) * tail_col[at, h : h + 1]).astype(BF)
            fresh = dot(keys[at, cols], weighted, ((0,), (0,)))
            held = running[cols, :]
            starts[b, cols, :] = held
            running[cols, :] = ends[h : h + 1, :] * held + fresh
        return 0

    lax.fori_loop(0, blocks, state_step, 0)
    state_out[0:local, :] = running[...].astype(BF)
    ends_total = cum_row[0][:, SPAN - 1 : SPAN]
    for b in range(1, blocks):
        ends_total = ends_total + cum_row[b][:, SPAN - 1 : SPAN]
    for h in range(heads):
        state_out[local + 16 * h : local + 16 * (h + 1), :] = jnp.broadcast_to(
            jnp.exp(ends_total[h : h + 1, :]), (16, DH)
        ).astype(BF)

    l_weights[2].wait()
    rotate_into(queries, project(0, 2), 0, None)

    def state_copy(step):
        return pltpu.make_async_remote_copy(
            src_ref=state_out,
            dst_ref=state_in.at[step - 1],
            send_sem=state_send.at[step - 1],
            recv_sem=state_recv.at[step - 1],
            device_id={"sp": lax.rem(sp + step, sp_count)},
        )

    for step in range(1, sp_count):
        @pl.when(sp + step < sp_count)
        def _():
            state_copy(step).start()

    rotate_into(queries, project(1, 2), 1, None)

    l_weights[3].wait()
    l_weights[4].wait()
    for c in range(2):
        first = project(c, 3).astype(BF).astype(F32)
        second = project(c, 4).astype(BF).astype(F32)
        gated[8 + c * half : 8 + (c + 1) * half, :] = (first * second).astype(BF).astype(F32)

    @pl.when(sp == 0)
    def _():
        gated[0:8, :] = jnp.zeros((8, local), F32)

    l_weights[5].wait()
    post[0:half, :] = project(0, 5).astype(BF)
    rim_copy = pltpu.make_async_remote_copy(
        src_ref=gated.at[pl.ds(rows, 8)],
        dst_ref=gated.at[pl.ds(0, 8)],
        send_sem=rim_send,
        recv_sem=rim_recv,
        device_id={"sp": lax.rem(sp + 1, sp_count)},
    )

    @pl.when(sp + 1 < sp_count)
    def _():
        rim_copy.start()

    post[half:, :] = project(1, 5).astype(BF)

    def inside_step(b, _):
        at = pl.ds(pl.multiple_of(b * SPAN, SPAN), SPAN)
        row = cum_row[b]
        for h in range(heads):
            cols = slice(h * DH, (h + 1) * DH)
            scores = dot(queries[at, cols], keys[at, cols], ((1,), (1,)))
            gap = jnp.minimum(cum_col[at, h : h + 1] - row[h : h + 1, :], 0.0)
            mix = (scores * jnp.where(lower, jnp.exp(gap), 0.0)).astype(BF)
            inside[at, cols] = dot(mix, values[at, cols])
        return 0

    lax.fori_loop(0, blocks, inside_step, 0)

    @pl.when(sp > 0)
    def _():
        rim_copy.wait_recv()

    l_taps.wait()
    tap = [taps[i : i + 1, :].astype(F32) for i in range(TAPS)]
    for b in range(blocks):
        base = b * SPAN + 8 - (TAPS - 1)
        convolved = tap[0] * gated[base : base + SPAN, :]
        for i in range(1, TAPS):
            convolved = convolved + tap[i] * gated[base + i : base + i + SPAN, :]
        at = slice(b * SPAN, (b + 1) * SPAN)
        conv_all[at, :] = (post[at, :].astype(F32) * convolved).astype(BF)

    def pair_copy(source, target, i):
        return pltpu.make_async_remote_copy(
            src_ref=source.at[pl.ds(pl.multiple_of(other * half, half), half)],
            dst_ref=target,
            send_sem=pair_send.at[i],
            recv_sem=pair_recv.at[i],
            device_id={"tp": other},
        )

    mine = pl.ds(pl.multiple_of(tp * half, half), half)
    my_inputs = pl.ds(pl.multiple_of(tp * local, local), local)
    other_inputs = pl.ds(pl.multiple_of(other * local, local), local)
    tiles = width // 512

    def tile_at(n):
        return pl.ds(pl.multiple_of(n * 512, 512), 512)

    l_woc.wait()
    conv_copy = pair_copy(conv_all, conv_in, 0)
    conv_copy.start()

    def conv_own(n, _):
        total[:, tile_at(n)] = dot(conv_all[mine, :], w_conv[my_inputs, tile_at(n)])
        return 0

    lax.fori_loop(0, tiles, conv_own, 0)
    conv_copy.wait_recv()

    def conv_other(n, _):
        total[:, tile_at(n)] += dot(conv_in[...], w_conv[other_inputs, tile_at(n)])
        return 0

    lax.fori_loop(0, tiles, conv_other, 0)

    for step in range(sp_count - 1, 0, -1):
        @pl.when(sp >= step)
        def _():
            state_copy(step).wait_recv()
            for h in range(heads):
                cols = slice(h * DH, (h + 1) * DH)
                shrink = state_in[step - 1, local + 16 * h : local + 16 * (h + 1), :].astype(F32)
                incoming[cols, :] = (
                    shrink[0:1, :] * incoming[cols, :] + state_in[step - 1, cols, :].astype(F32)
                )

    def across_half(which):
        def step(i, before):
            b = which * half_blocks + i
            at = pl.ds(pl.multiple_of(b * SPAN, SPAN), SPAN)
            factor = jnp.exp(before)
            for h in range(heads):
                cols = slice(h * DH, (h + 1) * DH)
                state = (starts[b, cols, :] + factor[h : h + 1, :] * incoming[cols, :]).astype(BF)
                across = dot(queries[at, cols], state)
                retained = inside[at, cols] + exp_col[at, h : h + 1] * across
                power = jnp.sum(retained * retained, axis=-1, keepdims=True) * (1.0 / DH)
                ret_all[at, cols] = (retained * lax.rsqrt(power + EPSILON)).astype(BF)
            return before + cum_row[b][:, SPAN - 1 : SPAN]

        first_half = cum_row[0][:, SPAN - 1 : SPAN]
        for b in range(1, half_blocks):
            first_half = first_half + cum_row[b][:, SPAN - 1 : SPAN]
        lax.fori_loop(0, half_blocks, step, first_half * which.astype(F32))

    across_half(other)
    ret_copy = pair_copy(ret_all, ret_in, 1)
    ret_copy.start()
    across_half(tp)
    l_wor.wait()

    def ret_own(n, _):
        total[:, tile_at(n)] += dot(ret_all[mine, :], w_ret[my_inputs, tile_at(n)])
        return 0

    lax.fori_loop(0, tiles, ret_own, 0)
    ret_copy.wait_recv()

    def ret_other(n, _):
        final = total[:, tile_at(n)] + dot(ret_in[...], w_ret[other_inputs, tile_at(n)])
        out_vmem[:, tile_at(n)] = final.astype(BF)
        return 0

    lax.fori_loop(0, tiles, ret_other, 0)

    for copy in tok_copies:
        copy.wait_send()
    for step in range(1, sp_count):
        @pl.when(sp + step < sp_count)
        def _():
            state_copy(step).wait_send()

    @pl.when(sp + 1 < sp_count)
    def _():
        rim_copy.wait_send()

    conv_copy.wait_send()
    ret_copy.wait_send()


def rotation_tables(sp_count, rows):
    halfway = DH // 2
    inverse = 10000.0 ** (-np.arange(halfway, dtype=np.float64) / halfway)
    sign = np.concatenate([-np.ones(halfway), np.ones(halfway)])
    inverse = np.concatenate([inverse, inverse])

    def table(positions):
        angles = positions[:, None] * inverse[None, :]
        return np.stack([np.cos(angles), np.sin(angles) * sign]).astype(np.float32)

    inner = table(np.arange(SPAN))
    blocks = rows // SPAN
    outer = np.zeros((sp_count, 2, -(-blocks // 8) * 8, DH), np.float32)
    for device in range(sp_count):
        outer[device, :, :blocks] = table(SPAN * (device * blocks + np.arange(blocks)))
    return jnp.asarray(inner), jnp.asarray(outer)


def body(
    sp_count,
    tokens,
    norm_gain,
    w_query,
    w_key,
    w_value,
    log_decay,
    w_conv_in,
    w_conv_pre,
    w_conv_post,
    conv_taps,
    w_out_ret,
    w_out_conv,
):
    rows, half_width = tokens.shape
    width = 2 * half_width
    heads = log_decay.shape[0]
    local = heads * DH
    half = rows // 2
    blocks = rows // SPAN
    inner, outer = rotation_tables(sp_count, rows)
    any_spec = pl.BlockSpec(memory_space=pltpu.HBM)
    vmem, dma = pltpu.VMEM, pltpu.SemaphoreType.DMA
    scratch = [
        vmem((2, rows, half_width), BF),
        vmem((rows, width), BF),
        vmem((6, width, local), BF),
        vmem(w_out_ret.shape, BF),
        vmem(w_out_conv.shape, BF),
        vmem((width,), BF),
        vmem(log_decay.shape, F32),
        vmem(conv_taps.shape, BF),
        vmem(inner.shape, F32),
        vmem(outer.shape[1:], F32),
        vmem((rows, DH), F32),
        vmem((rows, DH), F32),
        vmem((blocks, heads, SPAN), F32),
        vmem((rows, heads), F32),
        vmem((rows, heads), F32),
        vmem((rows, heads), F32),
        vmem((rows, local), BF),
        vmem((rows, local), BF),
        vmem((rows, local), BF),
        vmem((rows, local), BF),
        vmem((rows + 8, local), F32),
        vmem((blocks, local, DH), F32),
        vmem((local, DH), F32),
        vmem((local + 16 * heads, DH), BF),
        vmem((sp_count - 1, local + 16 * heads, DH), BF),
        vmem((local, DH), F32),
        vmem((rows, local), F32),
        vmem((rows, local), BF),
        vmem((half, local), BF),
        vmem((rows, local), BF),
        vmem((half, local), BF),
        vmem((half, width), F32),
        dma((13,)),
        dma((2,)),
        dma((2,)),
        dma((2,)),
        dma((sp_count - 1,)),
        dma((sp_count - 1,)),
        dma((2,)),
        dma((2,)),
        dma,
        dma,
    ]
    return pl.pallas_call(
        functools.partial(kernel, sp_count),
        out_shape=pltpu.VMEM((half, width), BF),
        in_specs=[any_spec] * 14,
        out_specs=pl.BlockSpec(memory_space=pltpu.VMEM),
        scratch_shapes=scratch,
        compiler_params=pltpu.CompilerParams(
            collective_id=0, has_side_effects=True, vmem_limit_bytes=65400000
        ),
        name="mixer",
    )(
        tokens,
        norm_gain,
        w_query,
        w_key,
        w_value,
        log_decay,
        w_conv_in,
        w_conv_pre,
        w_conv_post,
        conv_taps,
        w_out_ret,
        w_out_conv,
        inner,
        outer,
    )


def solution(mesh):
    in_specs = (
        P(("fs", "sp"), "tp"),
        P(),
        P(None, "tp"),
        P(None, "tp"),
        P(None, "tp"),
        P("tp", "sp"),
        P(None, "tp"),
        P(None, "tp"),
        P(None, "tp"),
        P(None, "tp"),
        P(),
        P(),
    )
    out_specs = P(("fs", "sp", "tp"), None)
    return jax.shard_map(
        functools.partial(body, mesh.shape["sp"]),
        mesh=mesh,
        in_specs=in_specs,
        out_specs=out_specs,
        check_vma=False,
    )
```
